32 devices in a mesh: ep: 16 (over z, y, x), tp: 2 (over core).
Axes of the slice: x: 2, y: 2, z: 4, core: 2. Of those that a mesh axis runs over, the one named last changes fastest.
Arguments:
- residual: bfloat16 [256, 2048], P(('ep', 'tp')), may hold values from -6 to 6
- query_latent: bfloat16 [256, 8, 512], P(('ep', 'tp')), may hold values from -40 to 40
- query_rotary: bfloat16 [256, 8, 32], P(('ep', 'tp')), may hold values from -6 to 6
- latent_new: bfloat16 [256, 512], P(('ep', 'tp')), may hold values from -16 to 16
- rotary_new: bfloat16 [256, 32], P(('ep', 'tp')), may hold values from -6 to 6
- latent_cache: bfloat16 [256, 256, 512], P(('ep', 'tp')), may hold values from -16 to 16
- rotary_cache: bfloat16 [256, 256, 32], P(('ep', 'tp')), may hold values from -6 to 6
- lengths: int32 [256], P(('ep', 'tp')), may hold values from 32 to 256, as said below
- value_up: bfloat16 [512, 8, 64], replicated, may hold values from -1 to 1
- out_proj: bfloat16 [512, 2048], replicated, may hold values from -0.5 to 0.5
- attn_gain: bfloat16 [2048], replicated, may hold values from 0.099609375 to 1.8984375
- mix_gate: bfloat16 [2048], replicated, may hold values from -0.125 to 0.125
- dense_w_gate: bfloat16 [2048, 2048], P(None, 'ep'), may hold values from -0.125 to 0.125
- dense_w_up: bfloat16 [2048, 2048], P(None, 'ep'), may hold values from -0.125 to 0.125
- dense_w_down: bfloat16 [2048, 2048], P('ep'), may hold values from -0.5 to 0.5
- expert_ids: int32 [256, 6], P(('ep', 'tp')), may hold values from 0 to 15, all different within a row; in each aligned block of 16 rows (0 to 15, 16 to 31, ...) at most 12 rows name the same one
- expert_scores: float32 [256, 6], P(('ep', 'tp')), may hold values from 0.1 to 5
- expert_gate: bfloat16 [16, 2048, 512], P('ep', None, 'tp'), may hold values from -0.125 to 0.125
- expert_up: bfloat16 [16, 2048, 512], P('ep', None, 'tp'), may hold values from -0.125 to 0.125
- expert_down: bfloat16 [16, 512, 2048], P('ep', 'tp'), may hold values from -1 to 1
- out_gain: bfloat16 [2048], replicated, may hold values from 0.099609375 to 1.8984375
Outputs:
- layer_out: bfloat16 [256, 2048], P(('ep', 'tp'))
The draws below stay inside these ranges and needn't reach their ends.
Inputs may be any that keep to these rules, and one draw needn't show every extreme that they name: `expert_ids`: within each aligned block of 16 rows (the sequences of one ep index) no expert is named by more than 12 rows, a bound that some block reaches; a row names 6 different experts. `lengths`: some sequence has exactly 256 cached positions.
All inputs are finite; a program needn't handle non-finite values.
Results may differ from the reference program's by a relative error of at most 0.018.
Values may be sent and summed in bfloat16 or wider, within the bound.
A program may use at most 128 MiB of HBM per device.

```python
import math
import jax
import jax.numpy as jnp
import numpy as np
from jax import lax

D = 2048
H = 8
KL = 512
ROPE = 32
NOPE = 64
V = 64
FE = 512
FD = 2048
TOPK = 6
SEQ_DEV = 8
CACHE = 256
EXPERTS = 16
TOK_GROUP = 16
SEQS = 256
CAP = 12
N_TP = 2


def draw_latent_cache(key, part):
    values = jnp.clip(jax.random.normal(jax.random.fold_in(key, 1), (SEQS, CACHE, KL), jnp.float32), -6.0, 6.0)
    return values.astype(jnp.bfloat16)


def draw_query_latent(key, part):
    values = 0.5 * jnp.clip(jax.random.normal(jax.random.fold_in(key, 2), (SEQS, H, KL), jnp.float32), -6.0, 6.0)
    return values.astype(jnp.bfloat16)


def draw_lengths(key, part):
    keys = jax.random.split(jax.random.fold_in(key, 3), 3)
    short = jax.random.randint(keys[0], (SEQS,), CACHE // 8, CACHE + 1)
    full = jax.random.randint(keys[1], (SEQS,), 0, 4) == 0
    values = jnp.where(full, CACHE, short)
    values = values.at[jax.random.randint(keys[2], (), 0, SEQS)].set(CACHE)
    return values.astype(jnp.int32)


def steps_of(own_key, dims, shards, low, top_value):
    level, own = 1.0, jax.random.fold_in(own_key, 6)
    for dim, shards_of in shards:
        steps = jnp.exp(jax.random.uniform(jax.random.fold_in(own, dim), (shards_of,), jnp.float32, low / len(shards), top_value / len(shards)))
        level = level * jnp.repeat(steps, dims[dim] // shards_of).reshape([-1 if axis == dim else 1 for axis in range(len(dims))])
    return level


def routed_block(stream_key, own, number, rows, count, top, bound, slope):
    ranking = jax.random.permutation(stream_key, count)
    crowded, common = portions_of(count, rows * top, bound, slope, True), portions_of(count, rows * top, bound, slope, False)
    places = jnp.arange(count)

    def named(tallies, rotation):
        used = int((tallies > 0).sum())
        fixed = max(1, used // 4)
        shifted = fixed + (places - fixed + rotation * (used - fixed)) % max(1, count - fixed)
        return jnp.zeros((count,), jnp.int32).at[ranking[jnp.where(places < fixed, places, shifted)]].set(jnp.asarray(tallies, jnp.int32))

    tallies = jnp.where(number % 4 == 0, named(crowded, number // 4), named(common, number - number // 4 - 1))
    mixed = jax.random.permutation(jax.random.fold_in(own, 3), count)
    giver, sink = mixed[0:count // 2 * 2:2], mixed[1:count // 2 * 2:2]
    room = jnp.minimum(tallies[giver] - 1, bound - tallies[sink]) // 2
    room = jnp.where((giver == ranking[0]) | (sink == ranking[0]) | (tallies[sink] == 0), 0, jnp.maximum(room, 0))
    shifted = jax.random.randint(jax.random.fold_in(own, 4), (count // 2,), 0, 1 << 20) % (room + 1)
    tallies = tallies.at[giver].add(-shifted).at[sink].add(shifted)
    labels = jnp.searchsorted(jnp.cumsum(tallies), jnp.arange(rows * top), side="right").astype(jnp.int32)
    table = labels.reshape(top, rows).T
    table = table[jax.random.permutation(jax.random.fold_in(own, 1), rows)]
    rotation = jax.random.randint(jax.random.fold_in(own, 2), (rows, 1), 0, top)
    return jnp.take_along_axis(table, (jnp.arange(top)[None, :] + rotation) % top, axis=1)


def portions_of(amount, total, limit, lean, full):
    portions = [(1 << 20) // math.isqrt(rank ** lean) + 1 for rank in range(1, amount + 1)]
    largest = limit if full else min(limit, max(-(-total // amount), total * portions[0] // sum(portions)))
    least = 1 if total - largest >= amount - 1 else 0
    holding, spare = [largest] + [least] * (amount - 1), total - largest - least * (amount - 1)
    while spare > 0:
        free = [i for i in range(1, amount) if holding[i] < largest] or [i for i in range(1, amount) if holding[i] < limit]
        pool, left = sum([portions[i] for i in free]), spare
        for i in free:
            extra = min(limit - holding[i], max(1, left * portions[i] // pool), spare)
            holding[i] = holding[i] + extra
            spare = spare - extra
    return np.array(holding)


def normal_values(own_key, dims, deviation, bound, cuts=(), kind=jnp.bfloat16):
    level = steps_of(own_key, dims, cuts, -0.22, 0.18) if cuts else 1.0
    values = jax.random.normal(own_key, dims, jnp.float32) * deviation * level
    return jnp.minimum(jnp.maximum(values, -bound), bound).astype(kind)


def setup_inputs(seed: int = 0) -> dict:
    splits = jax.random.split(jax.random.key(seed), 22)
    residual = normal_values(splits[0], (SEQS, D), 1.0, 6.0, ((0, 32),))
    query_latent = draw_query_latent(jax.random.fold_in(splits[21], 71), 0)
    query_rotary = normal_values(splits[2], (SEQS, H, ROPE), 1.0, 6.0, ((0, 32),))
    latent_new = normal_values(splits[3], (SEQS, KL), 3.0, 16.0, ((0, 32),))
    rotary_new = normal_values(splits[4], (SEQS, ROPE), 1.0, 6.0, ((0, 32),))
    latent_cache = draw_latent_cache(jax.random.fold_in(splits[21], 71), 0)
    rotary_cache = normal_values(splits[6], (SEQS, CACHE, ROPE), 1.0, 6.0, ((0, 32),))
    lengths = draw_lengths(jax.random.fold_in(splits[21], 71), 0)
    value_up = normal_values(splits[8], (KL, H, V), (KL // 16) ** -0.5, 1.0)
    out_proj = normal_values(splits[9], (H * V, D), (H * V // 4) ** -0.5, 0.5)
    attn_gain = jnp.clip(1.0 + 0.18 * jax.random.normal(splits[10], (D,), jnp.float32), 0.099609375, 1.8984375).astype(jnp.bfloat16)
    mix_gate = normal_values(splits[11], (D,), D ** -0.5, 0.125)
    dense_w_gate = normal_values(splits[12], (D, FD), D ** -0.5, 0.125, ((1, 16),))
    dense_w_up = normal_values(splits[13], (D, FD), D ** -0.5, 0.125, ((1, 16),))
    dense_w_down = normal_values(splits[14], (FD, D), (FD // 16) ** -0.5, 0.5, ((0, 16),))
    expert_ids_keys = jax.random.split(jax.random.fold_in(splits[15], 1), SEQS // TOK_GROUP)
    expert_ids_turns = jax.random.permutation(jax.random.fold_in(splits[15], 3), SEQS // TOK_GROUP)
    expert_ids = jax.vmap(lambda own, number: routed_block(jax.random.fold_in(splits[15], 2), own, number, TOK_GROUP, EXPERTS, TOPK, CAP, 2))(expert_ids_keys, expert_ids_turns).reshape((SEQS, TOPK))
    expert_scores = jnp.clip(jnp.exp(math.log(5.0) - 3.912023 * jax.random.uniform(splits[16], (SEQS, TOPK), jnp.float32) ** steps_of(splits[16], (SEQS, TOPK), ((0, 32),), -0.2, 0.2)), 0.1, 5.0)
    expert_gate = normal_values(splits[17], (EXPERTS, D, FE), D ** -0.5, 0.125, ((0, 16), (2, 2)))
    expert_up = normal_values(splits[18], (EXPERTS, D, FE), D ** -0.5, 0.125, ((0, 16), (2, 2)))
    expert_down = normal_values(splits[19], (EXPERTS, FE, D), (FE // 16) ** -0.5, 1.0, ((0, 16), (1, 2)))
    out_gain = jnp.clip(1.0 + 0.18 * jax.random.normal(splits[20], (D,), jnp.float32), 0.099609375, 1.8984375).astype(jnp.bfloat16)
    return dict(residual=residual, query_latent=query_latent, query_rotary=query_rotary, latent_new=latent_new, rotary_new=rotary_new, latent_cache=latent_cache, rotary_cache=rotary_cache, lengths=lengths, value_up=value_up, out_proj=out_proj, attn_gain=attn_gain, mix_gate=mix_gate, dense_w_gate=dense_w_gate, dense_w_up=dense_w_up, dense_w_down=dense_w_down, expert_ids=expert_ids, expert_scores=expert_scores, expert_gate=expert_gate, expert_up=expert_up, expert_down=expert_down, out_gain=out_gain)


ALPHA = 8.0 ** 0.25
EPS = 1e-06
ROPE_BASE = 10000.0

def rotate(vector, position):
    half_dim = vector.shape[-1] // 2
    inv_freq = ROPE_BASE ** (-jnp.arange(half_dim, dtype=jnp.float32) / half_dim)
    angles = position.astype(jnp.float32)[..., None] * inv_freq
    cosine = jnp.cos(angles)
    sine_part = jnp.sin(angles)
    lower_half = vector[..., :half_dim]
    upper_half = vector[..., half_dim:]
    return jnp.concatenate([lower_half * cosine - upper_half * sine_part, upper_half * cosine + lower_half * sine_part], axis=-1)

def normalize(values, gain):
    center = lax.optimization_barrier(jnp.mean(values, -1, keepdims=True))
    spread = lax.optimization_barrier(jnp.mean(jnp.square(values - center), -1, keepdims=True))
    return (values - center) * lax.rsqrt(spread + EPS) * gain.astype(jnp.float32)

def attend(block):
    query_latent, query_rotary, latent_new, rotary_new, latent_cache, rotary_cache, lengths = block
    score_scale = (NOPE + ROPE) ** (-0.5)
    query_turned = rotate(query_rotary.astype(jnp.float32), lengths[:, None]).astype(jnp.bfloat16)
    key_turned = rotate(rotary_new.astype(jnp.float32), lengths).astype(jnp.bfloat16)
    query_wide = query_latent.astype(jnp.float32)
    turned_wide = query_turned.astype(jnp.float32)
    cache_wide = latent_cache.astype(jnp.float32)
    new_wide = latent_new.astype(jnp.float32)
    scores = (jnp.einsum('bhr,btr->bht', query_wide, cache_wide) + jnp.einsum('bhe,bte->bht', turned_wide, rotary_cache.astype(jnp.float32))) * score_scale
    own_score = (jnp.einsum('bhr,br->bh', query_wide, new_wide) + jnp.einsum('bhe,be->bh', turned_wide, key_turned.astype(jnp.float32))) * score_scale
    live = jnp.arange(CACHE, dtype=jnp.int32)[None, :] < lengths[:, None]
    scores = jnp.where(live[:, None, :], scores, -jnp.inf)
    top_score = jnp.maximum(lax.optimization_barrier(jnp.max(scores, -1)), own_score)
    cache_probs = jnp.exp(scores - top_score[..., None])
    own_prob = jnp.exp(own_score - top_score)
    prob_total = lax.optimization_barrier(jnp.sum(cache_probs, -1)) + own_prob
    cache_weights = (cache_probs / prob_total[..., None]).astype(jnp.bfloat16)
    own_weight = (own_prob / prob_total).astype(jnp.bfloat16)
    latent_out = jnp.einsum('bht,btr->bhr', cache_weights.astype(jnp.float32), cache_wide) + own_weight.astype(jnp.float32)[..., None] * new_wide[:, None, :]
    return latent_out.astype(jnp.bfloat16)

def expert_block(block):
    token_rows, gate_weight, up_weight, down_weight = block
    flat_rows = token_rows.reshape(-1, D)
    half_width = FE // N_TP
    summed = jnp.zeros(flat_rows.shape, jnp.float32)
    for part_index in range(N_TP):
        lower = part_index * half_width
        upper = lower + half_width
        gate_pre = jnp.dot(flat_rows, gate_weight[:, lower:upper], preferred_element_type=jnp.float32)
        up_pre = jnp.dot(flat_rows, up_weight[:, lower:upper], preferred_element_type=jnp.float32)
        hidden_part = (jax.nn.silu(gate_pre) * up_pre).astype(jnp.bfloat16)
        part_out = jnp.dot(hidden_part, down_weight[lower:upper], preferred_element_type=jnp.float32).astype(jnp.bfloat16)
        summed = summed + part_out.astype(jnp.float32)
    return summed.astype(jnp.bfloat16).reshape(token_rows.shape)

def reference(residual, query_latent, query_rotary, latent_new, rotary_new, latent_cache, rotary_cache, lengths, value_up, out_proj, attn_gain, mix_gate, dense_w_gate, dense_w_up, dense_w_down, expert_ids, expert_scores, expert_gate, expert_up, expert_down, out_gain):
    block_count = SEQS // SEQ_DEV

    def split_blocks(array):
        return array.reshape((block_count, SEQ_DEV) + array.shape[1:])
    latent_out = lax.map(attend, (split_blocks(query_latent), split_blocks(query_rotary), split_blocks(latent_new), split_blocks(rotary_new), split_blocks(latent_cache), split_blocks(rotary_cache), split_blocks(lengths)))
    latent_out = latent_out.reshape(SEQS, H, KL)
    heads_out = jnp.einsum('bhr,rhv->bhv', latent_out.astype(jnp.float32), value_up.astype(jnp.float32))
    heads_out = heads_out.astype(jnp.bfloat16).reshape(SEQS, H * V)
    attn = jnp.dot(heads_out, out_proj, preferred_element_type=jnp.float32).astype(jnp.bfloat16)
    mixed = normalize(ALPHA * residual.astype(jnp.float32) + attn.astype(jnp.float32), attn_gain).astype(jnp.bfloat16)
    mix = jax.nn.sigmoid(jnp.dot(mixed, mix_gate, preferred_element_type=jnp.float32))
    gate_pre = jnp.dot(mixed, dense_w_gate, preferred_element_type=jnp.float32)
    up_pre = jnp.dot(mixed, dense_w_up, preferred_element_type=jnp.float32)
    hidden = (jax.nn.silu(gate_pre) * up_pre).astype(jnp.bfloat16)
    dense_out = jnp.dot(hidden, dense_w_down, preferred_element_type=jnp.float32).astype(jnp.bfloat16)
    group_count = SEQS // TOK_GROUP
    route_ids = expert_ids.reshape(group_count, TOK_GROUP * TOPK)
    onehot = (route_ids[..., None] == jnp.arange(EXPERTS, dtype=jnp.int32)).astype(jnp.int32)
    slot_index = lax.optimization_barrier(jnp.sum((jnp.cumsum(onehot, 1) - 1) * onehot, -1)).astype(jnp.int32)
    group_index = jnp.broadcast_to(jnp.arange(group_count, dtype=jnp.int32)[:, None], route_ids.shape)
    token_rows = jnp.repeat(mixed.reshape(group_count, TOK_GROUP, D), TOPK, axis=1)
    buffer = jnp.zeros((EXPERTS, group_count, CAP, D), jnp.bfloat16).at[route_ids, group_index, slot_index].set(token_rows)
    expert_out = lax.map(expert_block, (buffer, expert_gate, expert_up, expert_down))
    picked = expert_out[route_ids, group_index, slot_index].reshape(SEQS, TOPK, D)
    share = expert_scores / lax.optimization_barrier(jnp.sum(expert_scores, 1, keepdims=True))
    routed = lax.optimization_barrier(jnp.sum(picked.astype(jnp.float32) * share[:, :, None], 1))
    summed_total = ALPHA * mixed.astype(jnp.float32) + routed + mix[:, None] * dense_out.astype(jnp.float32)
    return normalize(summed_total, out_gain).astype(jnp.bfloat16)
```

```python
import functools
import math

import jax
import jax.numpy as jnp
from jax import lax
from jax.experimental import pallas as pl
from jax.experimental.pallas import tpu as pltpu
from jax.sharding import PartitionSpec as P

NOPE = 64
ALPHA = 8.0**0.25
EPS = 1e-06
ROPE_BASE = 10000.0
F32 = jnp.float32
BF16 = jnp.bfloat16
MESH = pl.DeviceIdType.MESH
VMEM = pltpu.VMEM


def normalize(values, gain):
    center = jnp.mean(values, -1, keepdims=True)
    shifted = values - center
    spread = jnp.mean(jnp.square(shifted), -1, keepdims=True)
    return shifted * lax.rsqrt(spread + EPS) * gain


def silu(value):
    return value / (1.0 + jnp.exp(-value))


def dot(a, b):
    return jnp.dot(a, b, preferred_element_type=F32)


def dot_nt(a, b):
    return lax.dot_general(a, b, (((1,), (1,)), ((), ())), preferred_element_type=F32)


def kernel(
    n,
    lengths,
    residual,
    query_latent,
    query_rotary,
    latent_new,
    rotary_new,
    vecs,
    ids,
    route_scores,
    rotary_cache,
    cache_hbm,
    vu_hbm,
    op_hbm,
    eg_hbm,
    eu_hbm,
    dg_hbm,
    du_hbm,
    ed_hbm,
    dd_hbm,
    out,
    cache,
    vu,
    op,
    eg,
    eu,
    dg,
    du,
    ed,
    dd,
    lat,
    gath,
    pout,
    pin,
    sbuf,
    rbuf,
    cache_sem,
    w_sem,
    ag_send,
    ag_recv,
    fw_send,
    fw_recv,
    p_sem,
    rs_send,
    rs_recv,
):
    me = lax.axis_index("ep")
    core = lax.axis_index("tp")
    other = 1 - core
    seqs, width = residual.shape
    heads = query_latent.shape[1]
    rope = query_rotary.shape[-1]
    cache_len = cache.shape[1]
    extra = gath.shape[-1] - width
    experts = n

    cache_copies = [
        pltpu.make_async_copy(cache_hbm.at[s], cache.at[s], cache_sem.at[s]) for s in range(seqs)
    ]
    for c in cache_copies:
        c.start()
    pairs = [
        (vu_hbm, vu),
        (op_hbm, op),
        (eg_hbm.at[0], eg),
        (eu_hbm.at[0], eu),
        (dg_hbm, dg),
        (du_hbm, du),
        (ed_hbm.at[0], ed),
        (dd_hbm, dd),
    ]
    w_copies = [pltpu.make_async_copy(a, b, w_sem.at[k]) for k, (a, b) in enumerate(pairs)]
    for c in w_copies:
        c.start()

    barrier = pltpu.get_barrier_semaphore()

    def greet(d, carry):
        pl.semaphore_signal(
            barrier, inc=1, device_id={"ep": lax.rem(me + d, n)}, device_id_type=MESH
        )
        return carry

    lax.fori_loop(1, n, greet, 0)
    pl.semaphore_signal(barrier, inc=1, device_id={"tp": other}, device_id_type=MESH)

    half = rope // 2
    lane = lax.broadcasted_iota(jnp.int32, (seqs, rope), 1)
    row = lax.broadcasted_iota(jnp.int32, (seqs, rope), 0)
    pos = jnp.zeros((seqs, rope), F32)
    for s in range(seqs):
        pos = jnp.where(row == s, lengths[s].astype(F32), pos)
    inv_freq = jnp.exp(lax.rem(lane, half).astype(F32) * (-math.log(ROPE_BASE) / half))
    angles = pos * inv_freq
    cosine = jnp.cos(angles)
    sine = jnp.sin(angles)
    ra = lax.broadcasted_iota(jnp.int32, (rope, rope), 0)
    rb = lax.broadcasted_iota(jnp.int32, (rope, rope), 1)
    swap = jnp.where(ra + half == rb, 1.0, jnp.where(ra == rb + half, -1.0, 0.0)).astype(BF16)
    q_rot = query_rotary[...].astype(F32).reshape(seqs * heads, rope)
    q_swap = dot(q_rot.astype(BF16), swap).reshape(seqs, heads, rope)
    q_rot = q_rot.reshape(seqs, heads, rope)
    k_rot = rotary_new[...]
    k_turn = (k_rot.astype(F32) * cosine + dot(k_rot, swap) * sine).astype(BF16).astype(F32)
    ln_all = latent_new[...].astype(F32)
    score_scale = (NOPE + rope) ** (-0.5)
    t_idx = lax.broadcasted_iota(jnp.int32, (heads, cache_len), 1)

    for s in range(seqs):
        q_turn = (q_rot[s] * cosine[s : s + 1] + q_swap[s] * sine[s : s + 1]).astype(BF16)
        ql = query_latent[s]
        own = (
            jnp.sum(ql.astype(F32) * ln_all[s : s + 1], -1, keepdims=True)
            + jnp.sum(q_turn.astype(F32) * k_turn[s : s + 1], -1, keepdims=True)
        ) * score_scale
        rot_part = dot_nt(q_turn, rotary_cache[s])
        cache_copies[s].wait()
        block = cache[s]
        scores = (dot_nt(ql, block) + rot_part) * score_scale
        scores = jnp.where(t_idx < lengths[s], scores, -jnp.inf)
        top = jnp.maximum(jnp.max(scores, -1, keepdims=True), own)
        probs = jnp.exp(scores - top)
        own_p = jnp.exp(own - top)
        total = jnp.sum(probs, -1, keepdims=True) + own_p
        weights = (probs / total).astype(BF16)
        own_w = (own_p / total).astype(BF16).astype(F32)
        lat[s * heads : (s + 1) * heads, :] = dot(weights, block) + own_w * ln_all[s : s + 1]

    w_copies[0].wait()
    w_copies[1].wait()
    wide = dot(lat[...].astype(BF16), vu[...])
    vdim = wide.shape[1] // heads
    wide = wide.reshape(seqs, heads, wide.shape[1])
    h_row = lax.broadcasted_iota(jnp.int32, wide.shape, 1)
    h_lane = lax.broadcasted_iota(jnp.int32, wide.shape, 2)
    own_head = (h_lane >= h_row * vdim) & (h_lane < (h_row + 1) * vdim)
    heads_out = jnp.sum(jnp.where(own_head, wide, 0.0), 1).astype(BF16)
    attn = dot(heads_out, op[...]).astype(BF16).astype(F32)
    mixed = normalize(ALPHA * residual[...].astype(F32) + attn, vecs[0:1, :]).astype(BF16)
    mixed_f = mixed.astype(F32)
    mix = 1.0 / (1.0 + jnp.exp(-jnp.sum(mixed_f * vecs[1:2, :], -1, keepdims=True)))

    sc = route_scores[...]
    share = sc / jnp.sum(sc, -1, keepdims=True)
    e_lane = lax.broadcasted_iota(jnp.int32, (seqs, extra), 1)
    low = e_lane > experts
    e_idx = jnp.where(low, e_lane - (experts + 1), e_lane)
    coef = jnp.where(e_idx == experts, mix, 0.0)
    for k in range(ids.shape[1]):
        coef = coef + jnp.where(e_idx == ids[:, k : k + 1], share[:, k : k + 1], 0.0)
    high = coef.astype(BF16)
    coef = jnp.where(low, coef - high.astype(F32), high.astype(F32)).astype(BF16)
    mine = gath.at[core, me]
    mine[:, :width] = mixed
    mine[:, width:] = coef

    pl.semaphore_wait(barrier, n)

    def ag_copy(d, block, target):
        return pltpu.make_async_remote_copy(
            src_ref=gath.at[core, block],
            dst_ref=gath.at[core, block],
            send_sem=ag_send.at[d],
            recv_sem=ag_recv.at[d],
            device_id={"ep": target},
            device_id_type=MESH,
        )

    def fw_copy(d, half_idx, block):
        return pltpu.make_async_remote_copy(
            src_ref=gath.at[half_idx, block],
            dst_ref=gath.at[half_idx, block],
            send_sem=fw_send.at[d],
            recv_sem=fw_recv.at[d],
            device_id={"tp": other},
            device_id_type=MESH,
        )

    def ag_start(d, carry):
        ag_copy(d, me, lax.rem(me + d, n)).start()
        return carry

    lax.fori_loop(1, n, ag_start, 0)
    fw_copy(0, core, me).start()
    for c in w_copies[2:]:
        c.wait()

    def ag_forward(d, carry):
        src = lax.rem(me + n - d, n)
        ag_copy(d, src, me).wait_recv()
        fw_copy(d, core, src).start()
        return carry

    lax.fori_loop(1, n, ag_forward, 0)

    chunk = 16
    rows = chunk * seqs

    def load(half_idx, b):
        block = gath[half_idx, pl.ds(b * chunk, chunk)]
        flat = block.astype(F32).reshape(rows, width + extra)
        x = flat[:, :width].astype(BF16)
        tail = flat[:, width:]
        c_lane = lax.broadcasted_iota(jnp.int32, (rows, extra), 1)
        pick = (c_lane == me) | (c_lane == me + experts + 1)
        weight = jnp.sum(jnp.where(pick, tail, 0.0), -1, keepdims=True)
        pick = (c_lane == experts) | (c_lane == 2 * experts + 1)
        blend = jnp.sum(jnp.where(pick, tail, 0.0), -1, keepdims=True)
        return x, weight, blend

    def expert_hidden(x, weight):
        return (silu(dot(x, eg[...])) * dot(x, eu[...]) * weight).astype(BF16)

    tile = 512 if width % 512 == 0 else width

    def fw_wait(d, carry):
        fw_copy(d, other, lax.rem(me + n - d, n)).wait_recv()
        return carry

    def partner_rows(b, carry):
        x, weight, _ = load(other, b)
        hidden = expert_hidden(x, weight)
        for t in range(0, width, tile):
            part = dot(hidden, ed[:, t : t + tile])
            pout[pl.ds(b * chunk, chunk), :, t : t + tile] = part.reshape(
                chunk, seqs, tile
            ).astype(BF16)
        return carry

    lax.fori_loop(0, n, fw_wait, 0)
    lax.fori_loop(0, n // chunk, partner_rows, 0)
    p_copy = pltpu.make_async_remote_copy(
        src_ref=pout,
        dst_ref=pin,
        send_sem=p_sem.at[0],
        recv_sem=p_sem.at[1],
        device_id={"tp": other},
        device_id_type=MESH,
    )
    p_copy.start()

    def own_hidden(b):
        x, weight, blend = load(core, b)
        hidden = expert_hidden(x, weight)
        d_hidden = (silu(dot(x, dg[...])) * dot(x, du[...]) * blend).astype(BF16)
        return hidden, d_hidden

    def own_rows(b, carry):
        hidden, d_hidden = own_hidden(b)
        for t in range(0, width, tile):
            part = dot(hidden, ed[:, t : t + tile]) + dot(d_hidden, dd[:, t : t + tile])
            part = part.reshape(chunk, seqs, tile)
            part = part + pin[pl.ds(b * chunk, chunk), :, t : t + tile].astype(F32)
            sbuf[pl.ds(b * chunk, chunk), :, t : t + tile] = part.astype(BF16)
        return carry

    p_copy.wait_recv()
    lax.fori_loop(0, n // chunk, own_rows, 0)

    def rs_copy(d, block, slot, target):
        return pltpu.make_async_remote_copy(
            src_ref=sbuf.at[block],
            dst_ref=rbuf.at[slot],
            send_sem=rs_send.at[d],
            recv_sem=rs_recv.at[d],
            device_id={"ep": target},
            device_id_type=MESH,
        )

    def rs_start(d, carry):
        target = lax.rem(me + d, n)
        rs_copy(d, target, d, target).start()
        return carry

    lax.fori_loop(1, n, rs_start, 0)
    start = ALPHA * mixed_f + sbuf[me].astype(F32)

    def rs_add(d, total):
        rs_copy(d, me, d, me).wait_recv()
        return total + rbuf[d].astype(F32)

    total = lax.fori_loop(1, n, rs_add, start)
    out[...] = normalize(total, vecs[2:3, :]).astype(BF16)

    def drain(d, carry):
        ag_copy(d, me, me).wait_send()
        rs_copy(d, me, d, me).wait_send()
        return carry

    def drain_fw(d, carry):
        fw_copy(d, core, me).wait_send()
        return carry

    lax.fori_loop(1, n, drain, 0)
    lax.fori_loop(0, n, drain_fw, 0)
    p_copy.wait_send()


def on_device(
    n,
    residual,
    query_latent,
    query_rotary,
    latent_new,
    rotary_new,
    latent_cache,
    rotary_cache,
    lengths,
    value_up,
    out_proj,
    attn_gain,
    mix_gate,
    dense_w_gate,
    dense_w_up,
    dense_w_down,
    expert_ids,
    expert_scores,
    expert_gate,
    expert_up,
    expert_down,
    out_gain,
):
    seqs, width = residual.shape
    heads = query_latent.shape[1]
    vu = value_up.reshape(value_up.shape[0], -1)
    vecs = jnp.stack([attn_gain, mix_gate, out_gain]).astype(F32)
    extra = -(-2 * (n + 1) // 128) * 128
    vmem = pl.BlockSpec(memory_space=VMEM)
    hbm = pl.BlockSpec(memory_space=pl.ANY)
    smem = pl.BlockSpec(memory_space=pltpu.SMEM)
    dma = pltpu.SemaphoreType.DMA
    block = (n, seqs, width)
    return pl.pallas_call(
        functools.partial(kernel, n),
        out_shape=jax.ShapeDtypeStruct((seqs, width), BF16),
        in_specs=[smem] + [vmem] * 9 + [hbm] * 9,
        out_specs=vmem,
        scratch_shapes=[
            VMEM(latent_cache.shape, BF16),
            VMEM(vu.shape, BF16),
            VMEM(out_proj.shape, BF16),
            VMEM(expert_gate.shape[1:], BF16),
            VMEM(expert_up.shape[1:], BF16),
            VMEM(dense_w_gate.shape, BF16),
            VMEM(dense_w_up.shape, BF16),
            VMEM(expert_down.shape[1:], BF16),
            VMEM(dense_w_down.shape, BF16),
            VMEM((seqs * heads, latent_cache.shape[-1]), F32),
            VMEM((2, n, seqs, width + extra), BF16),
            VMEM(block, BF16),
            VMEM(block, BF16),
            VMEM(block, BF16),
            VMEM(block, BF16),
            dma((seqs,)),
            dma((8,)),
            dma((n,)),
            dma((n,)),
            dma((n,)),
            dma((n,)),
            dma((2,)),
            dma((n,)),
            dma((n,)),
        ],
        compiler_params=pltpu.CompilerParams(
            collective_id=0, has_side_effects=True, vmem_limit_bytes=60 * 1024 * 1024
        ),
    )(
        lengths,
        residual,
        query_latent,
        query_rotary,
        latent_new,
        rotary_new,
        vecs,
        expert_ids,
        expert_scores,
        rotary_cache,
        latent_cache,
        vu,
        out_proj,
        expert_gate,
        expert_up,
        dense_w_gate,
        dense_w_up,
        expert_down,
        dense_w_down,
    )


def solution(mesh):
    rows = P(("ep", "tp"), None)
    rows3 = P(("ep", "tp"), None, None)
    return jax.shard_map(
        functools.partial(on_device, mesh.shape["ep"]),
        mesh=mesh,
        in_specs=(
            rows,
            rows3,
            rows3,
            rows,
            rows,
            rows3,
            rows3,
            P(("ep", "tp")),
            P(),
            P(),
            P(),
            P(),
            P(None, "ep"),
            P(None, "ep"),
            P("ep", None),
            rows,
            rows,
            P("ep", None, "tp"),
            P("ep", None, "tp"),
            P("ep", "tp", None),
            P(),
        ),
        out_specs=rows,
        check_vma=False,
    )
```

```python
import functools
import math

import jax
import jax.numpy as jnp
from jax import lax
from jax.experimental import pallas as pl
from jax.experimental.pallas import tpu as pltpu
from jax.sharding import PartitionSpec as P

NOPE = 64
ALPHA = 8.0**0.25
EPS = 1e-06
ROPE_BASE = 10000.0
F32 = jnp.float32
BF16 = jnp.bfloat16
MESH = pl.DeviceIdType.MESH
VMEM = pltpu.VMEM


def normalize(values, gain):
    center = jnp.mean(values, -1, keepdims=True)
    shifted = values - center
    spread = jnp.mean(jnp.square(shifted), -1, keepdims=True)
    return shifted * lax.rsqrt(spread + EPS) * gain


def vector(ref):
    return ref[...].astype(F32).reshape(1, ref.shape[0])


def inner_size(n):
    size = 1
    while size * size < n:
        size *= 2
    return size if n % size == 0 else n


def silu(value):
    return value / (1.0 + jnp.exp(-value))


def dot(a, b):
    return jnp.dot(a, b, preferred_element_type=F32)


def dot_nt(a, b):
    return lax.dot_general(a, b, (((1,), (1,)), ((), ())), preferred_element_type=F32)


def kernel(
    n,
    lengths,
    residual,
    query_latent,
    query_rotary,
    latent_new,
    rotary_new,
    attn_gain,
    mix_gate,
    out_gain,
    ids,
    route_scores,
    rotary_cache,
    cache_hbm,
    vu_hbm,
    op_hbm,
    eg_hbm,
    eu_hbm,
    dg_hbm,
    du_hbm,
    ed_hbm,
    dd_hbm,
    out,
    cache,
    vu,
    op,
    eg,
    eu,
    dg,
    du,
    ed,
    dd,
    lat,
    gath,
    pout,
    pin,
    sbuf,
    rbuf,
    zbuf,
    hid_own,
    hid_other,
    hid_dense,
    cache_sem,
    w_sem,
    ag_send,
    ag_recv,
    fw_send,
    fw_recv,
    p_send,
    p_recv,
    rs_send,
    rs_recv,
):
    me = lax.axis_index("ep")
    core = lax.axis_index("tp")
    other = 1 - core
    seqs, width = residual.shape
    heads = query_latent.shape[1]
    rope = query_rotary.shape[-1]
    cache_len = cache.shape[1]
    extra = gath.shape[-1] - width
    experts = n

    cache_copies = [
        pltpu.make_async_copy(cache_hbm.at[s], cache.at[s], cache_sem.at[s]) for s in range(seqs)
    ]
    for c in cache_copies:
        c.start()
    pairs = [
        (vu_hbm, vu),
        (op_hbm, op),
        (eg_hbm.at[0], eg),
        (eu_hbm.at[0], eu),
        (dg_hbm, dg),
        (du_hbm, du),
        (ed_hbm.at[0], ed),
        (dd_hbm, dd),
    ]
    w_copies = [pltpu.make_async_copy(a, b, w_sem.at[k]) for k, (a, b) in enumerate(pairs)]
    for c in w_copies:
        c.start()

    barrier = pltpu.get_barrier_semaphore()

    inner = inner_size(n)
    outer = n // inner
    zo = lax.div(me, inner)
    xi = lax.rem(me, inner)

    def ahead(dz, dx):
        return lax.rem(zo + dz, outer) * inner + lax.rem(xi + dx, inner)

    def behind(dz, dx):
        return ahead(outer - dz, inner - dx)

    def greet_outer(d, carry):
        pl.semaphore_signal(barrier, inc=1, device_id={"ep": ahead(d, 0)}, device_id_type=MESH)
        return carry

    def greet_inner(d, carry):
        pl.semaphore_signal(barrier, inc=1, device_id={"ep": ahead(0, d)}, device_id_type=MESH)
        return carry

    lax.fori_loop(1, outer, greet_outer, 0)
    lax.fori_loop(1, inner, greet_inner, 0)
    pl.semaphore_signal(barrier, inc=1, device_id={"tp": other}, device_id_type=MESH)

    half = rope // 2
    lane = lax.broadcasted_iota(jnp.int32, (seqs, rope), 1)
    row = lax.broadcasted_iota(jnp.int32, (seqs, rope), 0)
    pos = jnp.zeros((seqs, rope), F32)
    for s in range(seqs):
        pos = jnp.where(row == s, lengths[s].astype(F32), pos)
    inv_freq = jnp.exp(lax.rem(lane, half).astype(F32) * (-math.log(ROPE_BASE) / half))
    angles = pos * inv_freq
    cosine = jnp.cos(angles)
    sine = jnp.sin(angles)
    ra = lax.broadcasted_iota(jnp.int32, (rope, rope), 0)
    rb = lax.broadcasted_iota(jnp.int32, (rope, rope), 1)
    swap = jnp.where(ra + half == rb, 1.0, jnp.where(ra == rb + half, -1.0, 0.0)).astype(BF16)
    q_rot = query_rotary[...].astype(F32).reshape(seqs * heads, rope)
    q_swap = dot(q_rot.astype(BF16), swap).reshape(seqs, heads, rope)
    q_rot = q_rot.reshape(seqs, heads, rope)
    k_rot = rotary_new[...]
    k_turn = (k_rot.astype(F32) * cosine + dot(k_rot, swap) * sine).astype(BF16).astype(F32)
    ln_all = latent_new[...].astype(F32)
    score_scale = (NOPE + rope) ** (-0.5)
    t_idx = lax.broadcasted_iota(jnp.int32, (heads, cache_len), 1)

    score_rows, own_rows_all = [], []
    for s in range(seqs):
        q_turn = (q_rot[s] * cosine[s : s + 1] + q_swap[s] * sine[s : s + 1]).astype(BF16)
        ql = query_latent[s]
        own_rows_all.append(
            jnp.sum(ql.astype(F32) * ln_all[s : s + 1], -1, keepdims=True)
            + jnp.sum(q_turn.astype(F32) * k_turn[s : s + 1], -1, keepdims=True)
        )
        rot_part = dot(q_turn, rotary_cache[s])
        cache_copies[s].wait()
        part = dot_nt(ql, cache[s]) + rot_part
        score_rows.append(jnp.where(t_idx < lengths[s], part, -jnp.inf))
    own = jnp.concatenate(own_rows_all, 0) * score_scale
    scores = jnp.concatenate(score_rows, 0) * score_scale
    top = jnp.maximum(jnp.max(scores, -1, keepdims=True), own)
    probs = jnp.exp(scores - top)
    own_p = jnp.exp(own - top)
    total = jnp.sum(probs, -1, keepdims=True) + own_p
    weights = probs / total
    own_w = (own_p / total).astype(BF16).astype(F32)
    for s in range(seqs):
        at = slice(s * heads, (s + 1) * heads)
        lat[at, :] = dot(weights[at].astype(BF16), cache[s]) + own_w[at] * ln_all[s : s + 1]

    w_copies[0].wait()
    w_copies[1].wait()
    wide = dot_nt(lat[...].astype(BF16), vu[...])
    vdim = wide.shape[1] // heads
    wide = wide.reshape(seqs, heads, wide.shape[1])
    h_row = lax.broadcasted_iota(jnp.int32, wide.shape, 1)
    h_lane = lax.broadcasted_iota(jnp.int32, wide.shape, 2)
    own_head = (h_lane >= h_row * vdim) & (h_lane < (h_row + 1) * vdim)
    heads_out = jnp.sum(jnp.where(own_head, wide, 0.0), 1).astype(BF16)
    attn = dot(heads_out, op[...]).astype(BF16).astype(F32)
    mixed = normalize(ALPHA * residual[...].astype(F32) + attn, vector(attn_gain)).astype(BF16)
    mixed_f = mixed.astype(F32)
    mix = 1.0 / (1.0 + jnp.exp(-jnp.sum(mixed_f * vector(mix_gate), -1, keepdims=True)))

    sc = route_scores[...]
    share = sc / jnp.sum(sc, -1, keepdims=True)
    e_lane = lax.broadcasted_iota(jnp.int32, (seqs, extra), 1)
    low = e_lane > experts
    e_idx = jnp.where(low, e_lane - (experts + 1), e_lane)
    coef = jnp.where(e_idx == experts, mix, 0.0)
    for k in range(ids.shape[1]):
        coef = coef + jnp.where(e_idx == ids[:, k : k + 1], share[:, k : k + 1], 0.0)
    high = coef.astype(BF16)
    coef = jnp.where(low, coef - high.astype(F32), high.astype(F32)).astype(BF16)
    mine = gath.at[core, me]
    mine[:, :width] = mixed
    mine[:, width:] = coef

    pl.semaphore_wait(barrier, outer + inner - 1)

    def ag_copy(slot, block, target):
        return pltpu.make_async_remote_copy(
            src_ref=gath.at[core, block],
            dst_ref=gath.at[core, block],
            send_sem=ag_send.at[slot],
            recv_sem=ag_recv.at[slot],
            device_id={"ep": target},
            device_id_type=MESH,
        )

    def fw_copy(d, half_idx, block):
        return pltpu.make_async_remote_copy(
            src_ref=gath.at[half_idx, block],
            dst_ref=gath.at[half_idx, block],
            send_sem=fw_send.at[d],
            recv_sem=fw_recv.at[d],
            device_id={"tp": other},
            device_id_type=MESH,
        )

    def ag_outer(d, carry):
        ag_copy(d * inner, me, ahead(d, 0)).start()
        return carry

    def ag_inner(dz, block):
        def send(d, carry):
            ag_copy(dz * inner + d, block, ahead(0, d)).start()
            return carry

        lax.fori_loop(1, inner, send, 0)

    lax.fori_loop(1, outer, ag_outer, 0)
    ag_inner(0, me)
    fw_copy(0, core, me).start()

    def ag_relay(dz, carry):
        block = behind(dz, 0)
        ag_copy(dz * inner, block, me).wait_recv()
        ag_inner(dz, block)
        fw_copy(dz * inner, core, block).start()
        return carry

    lax.fori_loop(1, outer, ag_relay, 0)

    def ag_forward(dz, carry):
        def one(dx, inside):
            block = behind(dz, dx)
            ag_copy(dz * inner + dx, block, me).wait_recv()
            fw_copy(dz * inner + dx, core, block).start()
            return inside

        return lax.fori_loop(1, inner, one, carry)

    lax.fori_loop(0, outer, ag_forward, 0)
    for c in w_copies[2:6]:
        c.wait()

    chunk = min(n, 16)
    rows = chunk * seqs

    def load(half_idx, b):
        block = gath[half_idx, pl.ds(b * chunk, chunk)]
        flat = block.astype(F32).reshape(rows, width + extra)
        x = flat[:, :width].astype(BF16)
        tail = flat[:, width:]
        c_lane = lax.broadcasted_iota(jnp.int32, (rows, extra), 1)
        pick = (c_lane == me) | (c_lane == me + experts + 1)
        weight = jnp.sum(jnp.where(pick, tail, 0.0), -1, keepdims=True)
        pick = (c_lane == experts) | (c_lane == 2 * experts + 1)
        blend = jnp.sum(jnp.where(pick, tail, 0.0), -1, keepdims=True)
        return x, weight, blend

    def expert_hidden(x, weight):
        return (silu(dot(x, eg[...])) * dot(x, eu[...]) * weight).astype(BF16)

    def own_hidden(b, carry):
        x, weight, blend = load(core, b)
        at = pl.ds(b * rows, rows)
        hid_own[at, :] = expert_hidden(x, weight)
        hid_dense[at, :] = (silu(dot(x, dg[...])) * dot(x, du[...]) * blend).astype(BF16)
        return carry

    lax.fori_loop(0, n // chunk, own_hidden, 0)

    def fw_wait(d, carry):
        fw_copy(d, other, behind(lax.div(d, inner), lax.rem(d, inner))).wait_recv()
        return carry

    lax.fori_loop(0, n, fw_wait, 0)

    def partner_hidden(b, carry):
        x, weight, _ = load(other, b)
        hid_other[pl.ds(b * rows, rows), :] = expert_hidden(x, weight)
        return carry

    lax.fori_loop(0, n // chunk, partner_hidden, 0)
    for c in w_copies[6:]:
        c.wait()
    tiles, tile = sbuf.shape[0], sbuf.shape[-1]

    def p_copy(t):
        return pltpu.make_async_remote_copy(
            src_ref=pout.at[t],
            dst_ref=pin.at[t],
            send_sem=p_send.at[t],
            recv_sem=p_recv.at[t],
            device_id={"tp": other},
            device_id_type=MESH,
        )

    def rs_inner(t, slot, block, target):
        return pltpu.make_async_remote_copy(
            src_ref=sbuf.at[t, block],
            dst_ref=rbuf.at[t, slot],
            send_sem=rs_send.at[t, slot],
            recv_sem=rs_recv.at[t, slot],
            device_id={"ep": target},
            device_id_type=MESH,
        )

    def rs_outer(t, d, target):
        return pltpu.make_async_remote_copy(
            src_ref=zbuf.at[t, d],
            dst_ref=rbuf.at[t, d * inner],
            send_sem=rs_send.at[t, d * inner],
            recv_sem=rs_recv.at[t, d * inner],
            device_id={"ep": target},
            device_id_type=MESH,
        )

    for t in range(tiles):
        cols = slice(t * tile, (t + 1) * tile)

        def partner_rows(b, carry):
            part = dot(hid_other[pl.ds(b * rows, rows), :], ed[:, cols])
            pout[t, pl.ds(b * chunk, chunk)] = part.reshape(chunk, seqs, tile).astype(BF16)
            return carry

        lax.fori_loop(0, n // chunk, partner_rows, 0)
        p_copy(t).start()

    for t in range(tiles):
        cols = slice(t * tile, (t + 1) * tile)
        p_copy(t).wait_recv()

        def own_rows(b, carry):
            at = pl.ds(b * rows, rows)
            part = dot(hid_own[at, :], ed[:, cols]) + dot(hid_dense[at, :], dd[:, cols])
            part = part.reshape(chunk, seqs, tile)
            part = part + pin[t, pl.ds(b * chunk, chunk)].astype(F32)
            sbuf[t, pl.ds(b * chunk, chunk)] = part.astype(BF16)
            return carry

        lax.fori_loop(0, n // chunk, own_rows, 0)

        def rs_start(k, carry):
            dz = outer - 1 - k

            def one(dx, inside):
                rs_inner(t, dz * inner + dx, ahead(dz, dx), ahead(0, dx)).start()
                return inside

            return lax.fori_loop(1, inner, one, carry)

        lax.fori_loop(0, outer, rs_start, 0)

    def inner_sum(t, dz, start):
        def one(dx, total):
            rs_inner(t, dz * inner + dx, me, me).wait_recv()
            return total + rbuf[t, dz * inner + dx].astype(F32)

        return lax.fori_loop(1, inner, one, start)

    for t in range(tiles):

        def rs_relay(k, carry):
            dz = outer - k
            value = inner_sum(t, dz, sbuf[t, ahead(dz, 0)].astype(F32))
            zbuf[t, dz] = value.astype(BF16)
            rs_outer(t, dz, ahead(dz, 0)).start()
            return carry

        lax.fori_loop(1, outer, rs_relay, 0)

    sums = []
    for t in range(tiles):
        cols = slice(t * tile, (t + 1) * tile)
        start = ALPHA * mixed_f[:, cols] + sbuf[t, me].astype(F32)
        value = inner_sum(t, 0, start)

        def outer_add(d, total):
            rs_outer(t, d, me).wait_recv()
            return total + rbuf[t, d * inner].astype(F32)

        sums.append(lax.fori_loop(1, outer, outer_add, value))
    total = jnp.concatenate(sums, axis=-1)
    out[...] = normalize(total, vector(out_gain)).astype(BF16)

    def drain(d, carry):
        ag_copy(d, me, me).wait_send()
        for t in range(tiles):
            rs_inner(t, d, me, me).wait_send()
        return carry

    def drain_fw(d, carry):
        fw_copy(d, core, me).wait_send()
        return carry

    lax.fori_loop(1, n, drain, 0)
    lax.fori_loop(0, n, drain_fw, 0)
    for t in range(tiles):
        p_copy(t).wait_send()


def on_device(
    n,
    residual,
    query_latent,
    query_rotary,
    latent_new,
    rotary_new,
    latent_cache,
    rotary_cache,
    lengths,
    value_up,
    out_proj,
    attn_gain,
    mix_gate,
    dense_w_gate,
    dense_w_up,
    dense_w_down,
    expert_ids,
    expert_scores,
    expert_gate,
    expert_up,
    expert_down,
    out_gain,
):
    seqs, width = residual.shape
    heads = query_latent.shape[1]
    vu = value_up.transpose(1, 2, 0).reshape(-1, value_up.shape[0])
    rotary_turned = rotary_cache.transpose(0, 2, 1)
    extra = -(-2 * (n + 1) // 128) * 128
    vmem = pl.BlockSpec(memory_space=VMEM)
    hbm = pl.BlockSpec(memory_space=pl.ANY)
    smem = pl.BlockSpec(memory_space=pltpu.SMEM)
    dma = pltpu.SemaphoreType.DMA
    tile = 512 if width % 512 == 0 else width
    tiles = width // tile
    block = (tiles, n, seqs, tile)
    return pl.pallas_call(
        functools.partial(kernel, n),
        out_shape=jax.ShapeDtypeStruct((seqs, width), BF16),
        in_specs=[smem] + [vmem] * 11 + [hbm] * 9,
        out_specs=vmem,
        scratch_shapes=[
            VMEM(latent_cache.shape, BF16),
            VMEM(vu.shape, BF16),
            VMEM(out_proj.shape, BF16),
            VMEM(expert_gate.shape[1:], BF16),
            VMEM(expert_up.shape[1:], BF16),
            VMEM(dense_w_gate.shape, BF16),
            VMEM(dense_w_up.shape, BF16),
            VMEM(expert_down.shape[1:], BF16),
            VMEM(dense_w_down.shape, BF16),
            VMEM((seqs * heads, latent_cache.shape[-1]), F32),
            VMEM((2, n, seqs, width + extra), BF16),
            VMEM(block, BF16),
            VMEM(block, BF16),
            VMEM(block, BF16),
            VMEM(block, BF16),
            VMEM((tiles, n // inner_size(n), seqs, tile), BF16),
            VMEM((n * seqs, expert_gate.shape[-1]), BF16),
            VMEM((n * seqs, expert_gate.shape[-1]), BF16),
            VMEM((n * seqs, dense_w_gate.shape[-1]), BF16),
            dma((seqs,)),
            dma((8,)),
            dma((n,)),
            dma((n,)),
            dma((n,)),
            dma((n,)),
            dma((tiles,)),
            dma((tiles,)),
            dma((tiles, n)),
            dma((tiles, n)),
        ],
        compiler_params=pltpu.CompilerParams(
            collective_id=0, has_side_effects=True, vmem_limit_bytes=60 * 1024 * 1024
        ),
    )(
        lengths,
        residual,
        query_latent,
        query_rotary,
        latent_new,
        rotary_new,
        attn_gain,
        mix_gate,
        out_gain,
        expert_ids,
        expert_scores,
        rotary_turned,
        latent_cache,
        vu,
        out_proj,
        expert_gate,
        expert_up,
        dense_w_gate,
        dense_w_up,
        expert_down,
        dense_w_down,
    )


def solution(mesh):
    rows = P(("ep", "tp"), None)
    rows3 = P(("ep", "tp"), None, None)
    return jax.shard_map(
        functools.partial(on_device, mesh.shape["ep"]),
        mesh=mesh,
        in_specs=(
            rows,
            rows3,
            rows3,
            rows,
            rows,
            rows3,
            rows3,
            P(("ep", "tp")),
            P(),
            P(),
            P(),
            P(),
            P(None, "ep"),
            P(None, "ep"),
            P("ep", None),
            rows,
            rows,
            P("ep", None, "tp"),
            P("ep", None, "tp"),
            P("ep", "tp", None),
            P(),
        ),
        out_specs=rows,
        check_vma=False,
    )
```
